512 devices in a mesh: grp: 2 (over y), tp: 16 (over z), dp: 16 (over x, core).
Axes of the slice: x: 8, y: 2, z: 16, core: 2. Of those that a mesh axis runs over, the one named last changes fastest.
The devices are a block of a 8x16x16 slice.
Arguments:
- tokens: bfloat16 [256, 4096], P(('grp', 'tp'), 'dp'), parts along dimension 0, may hold values from -50 to 50
- norm_gain: float32 [2, 4096], P(None, 'dp'), may hold values from 0.1 to 1.9
- query_weight: bfloat16 [2, 4096, 4096], P(None, 'dp', 'tp'), may hold values from -0.09375 to 0.09375
- key_weight: bfloat16 [2, 4096, 4096], P(None, 'dp', 'tp'), may hold values from -0.09375 to 0.09375
- value_weight: bfloat16 [2, 4096, 4096], P(None, 'dp', 'tp'), may hold values from -0.09375 to 0.09375
- outgate_weight: bfloat16 [2, 4096, 4096], P(None, 'dp', 'tp'), may hold values from -0.09375 to 0.09375
- input_gate_weight: bfloat16 [2, 4096, 64], P(None, 'dp', 'tp'), may hold values from -0.09375 to 0.09375
- forget_gate_weight: bfloat16 [2, 4096, 64], P(None, 'dp', 'tp'), may hold values from -0.09375 to 0.09375
- forget_bias: float32 [2, 64], P(None, 'tp'), may hold values from -2 to 5
- out_weight: bfloat16 [2, 4096, 4096], P(None, 'tp', 'dp'), may hold values from -0.09375 to 0.09375
- memory_state: float32 [2, 256, 64, 4096], P(None, ('grp', 'dp'), 'tp'), parts along dimension 1, may hold values from -0.9 to 0.9
- normalizer_state: float32 [2, 256, 4096], P(None, ('grp', 'dp'), 'tp'), parts along dimension 1, may hold values from -0.9 to 0.9
- maximum_state: float32 [2, 256, 64], P(None, ('grp', 'dp'), 'tp'), parts along dimension 1, may hold values from -1 to 1
Outputs:
- next_tokens: bfloat16 [256, 4096], P(('grp', 'tp'), 'dp'), parts along dimension 0
- next_memory: float32 [2, 256, 64, 4096], P(None, ('grp', 'dp'), 'tp'), parts along dimension 1
- next_normalizer: float32 [2, 256, 4096], P(None, ('grp', 'dp'), 'tp'), parts along dimension 1
- next_maximum: float32 [2, 256, 64], P(None, ('grp', 'dp'), 'tp'), parts along dimension 1
The draws below stay inside these ranges and needn't reach their ends.
There are 2 independent parts, one for each index of `grp`. The reference program is written for one: setup_inputs(seed, part) draws one part's arguments, and reference() takes and returns one part's arrays. A program takes and returns all parts, laid end to end along the dimension named above; an argument that names none is the same for every part. Nothing has to cross between parts.
All inputs are finite; a program needn't handle non-finite values.
Results may differ from the reference program's by a relative error of at most 0.0074.
Values may be sent and summed in bfloat16 or wider, within the bound.
A program may use at most 64 MiB of HBM per device.

```python
import math
import jax
import jax.numpy as jnp
from jax import lax

D = 4096
HEADS = 64
HEAD = 64
LAYERS = 2
BATCH = 128


def draw_tokens(key, part):
    key_entries = jax.random.fold_in(key, 11)
    key_rows = jax.random.fold_in(key, 12)
    columns = jnp.arange(D, dtype=jnp.float32) / (D - 1) - 0.5
    row_scale = jnp.exp(jax.random.uniform(key_rows, (BATCH, 1), jnp.float32, -1.15, 1.15))
    entries = jnp.clip(jax.random.normal(key_entries, (BATCH, D), jnp.float32), -5.0, 5.0)
    column_ramp = jnp.exp(math.log(10.0) * columns)
    return (entries * row_scale * column_ramp[None, :]).astype(jnp.bfloat16)


def levels(rng, extent, pieces, least, largest):
    def one(position, shards_of):
        steps = jax.random.uniform(jax.random.fold_in(jax.random.fold_in(rng, 6), position), (shards_of,), jnp.float32, least / len(pieces), largest / len(pieces))
        return jnp.repeat(jnp.exp(steps), extent[position] // shards_of).reshape((-1,) + (1,) * (len(extent) - position - 1))

    level = one(*pieces[0])
    for cut in pieces[1:]:
        level = level * one(*cut)
    return level


def scatter_about(key, dims, width, bound, cuts=(), kind=jnp.bfloat16):
    drawn = width * jax.random.normal(key, dims, jnp.float32)
    if cuts:
        drawn = drawn * levels(key, dims, cuts, -0.22, 0.18)
    return jnp.clip(drawn, -bound, bound).astype(kind)


def setup_inputs(seed: int = 0, part: int = 0) -> dict:
    streams_of = jax.random.split(jax.random.key(seed), 14)
    own_keys = jax.random.split(jax.random.fold_in(streams_of[13], part), 14)
    return {
        "tokens": draw_tokens(jax.random.fold_in(jax.random.fold_in(streams_of[13], part), 71), part),
        "norm_gain": jnp.clip(1.0 + 0.18 * jax.random.normal(streams_of[1], (LAYERS, D), jnp.float32), 0.1, 1.9),
        "query_weight": scatter_about(streams_of[2], (LAYERS, D, HEADS * HEAD), D ** -0.5, 0.09375, ((1, 16), (2, 16))),
        "key_weight": scatter_about(streams_of[3], (LAYERS, D, HEADS * HEAD), D ** -0.5, 0.09375, ((1, 16), (2, 16))),
        "value_weight": scatter_about(streams_of[4], (LAYERS, D, HEADS * HEAD), D ** -0.5, 0.09375, ((1, 16), (2, 16))),
        "outgate_weight": scatter_about(streams_of[5], (LAYERS, D, HEADS * HEAD), D ** -0.5, 0.09375, ((1, 16), (2, 16))),
        "input_gate_weight": scatter_about(streams_of[6], (LAYERS, D, HEADS), D ** -0.5, 0.09375, ((1, 16), (2, 16))),
        "forget_gate_weight": scatter_about(streams_of[7], (LAYERS, D, HEADS), D ** -0.5, 0.09375, ((1, 16), (2, 16))),
        "forget_bias": jnp.clip(-2.0 + 7.0 * jax.random.uniform(streams_of[8], (LAYERS, HEADS), jnp.float32) ** levels(streams_of[8], (LAYERS, HEADS), ((1, 16),), -0.2, 0.2), -2.0, 5.0),
        "out_weight": scatter_about(streams_of[9], (LAYERS, HEADS * HEAD, D), (HEADS * HEAD) ** -0.5, 0.09375, ((1, 16), (2, 16))),
        "memory_state": scatter_about(own_keys[10], (LAYERS, BATCH, HEADS, HEAD * HEAD), 0.15, 0.9, ((1, 16), (2, 16)), jnp.float32),
        "normalizer_state": scatter_about(own_keys[11], (LAYERS, BATCH, HEADS * HEAD), 0.15, 0.9, ((1, 16), (2, 16)), jnp.float32),
        "maximum_state": jnp.clip(jax.random.uniform(own_keys[12], (LAYERS, BATCH, HEADS), jnp.float32, -1.0, 1.0) * levels(own_keys[12], (LAYERS, BATCH, HEADS), ((1, 16), (2, 16)), -0.4, 0.0), -1.0, 1.0),
    }


EPS = 1e-06

def reference(tokens, norm_gain, query_weight, key_weight, value_weight, outgate_weight, input_gate_weight, forget_gate_weight, forget_bias, out_weight, memory_state, normalizer_state, maximum_state):
    current = tokens
    memories = []
    normalizers = []
    maxima = []
    batch_rows = tokens.shape[0]
    shape = (batch_rows, HEADS, HEAD)
    for layer_idx in range(LAYERS):
        x_float = current.astype(jnp.float32)
        squares = lax.optimization_barrier(jnp.sum(x_float * x_float, axis=1))
        inv_rms = lax.rsqrt(squares / D + EPS)[:, None]
        scaled = (x_float * norm_gain[layer_idx][None, :]).astype(jnp.bfloat16)

        def project(weight):
            return inv_rms * jnp.dot(scaled, weight, preferred_element_type=jnp.float32)

        def rounded(weight):
            stored = lax.optimization_barrier(project(weight).astype(jnp.bfloat16))
            return stored.astype(jnp.float32).reshape(shape)
        query_vec = rounded(query_weight[layer_idx])
        key_vec = rounded(key_weight[layer_idx]) * HEAD ** (-0.5)
        value_vec = rounded(value_weight[layer_idx])
        gate_vec = rounded(outgate_weight[layer_idx])
        input_pre = project(input_gate_weight[layer_idx])
        forget_pre = project(forget_gate_weight[layer_idx]) + forget_bias[layer_idx][None, :]
        log_forget = jax.nn.log_sigmoid(forget_pre)
        old_max = maximum_state[layer_idx]
        new_max = jnp.maximum(log_forget + old_max, input_pre)
        keep_rate = jnp.exp(log_forget + old_max - new_max)
        admit_rate = jnp.exp(input_pre - new_max)
        memory = memory_state[layer_idx].reshape(batch_rows, HEADS, HEAD, HEAD)
        memory = keep_rate[:, :, None, None] * memory + admit_rate[:, :, None, None] * key_vec[:, :, :, None] * value_vec[:, :, None, :]
        normalizer = keep_rate[:, :, None] * normalizer_state[layer_idx].reshape(shape) + admit_rate[:, :, None] * key_vec
        numerator = jnp.einsum('bhd,bhde->bhe', query_vec, memory, precision=lax.Precision.HIGHEST)
        denominator = lax.optimization_barrier(jnp.sum(query_vec * normalizer, axis=2))
        readout = numerator / jnp.maximum(jnp.abs(denominator), jnp.exp(-new_max))[:, :, None]
        mixed = (readout * jax.nn.sigmoid(gate_vec)).astype(jnp.bfloat16).reshape(batch_rows, HEADS * HEAD)
        summed = jnp.dot(mixed, out_weight[layer_idx], preferred_element_type=jnp.float32)
        current = (x_float + summed).astype(jnp.bfloat16)
        memories.append(memory.reshape(batch_rows, HEADS, HEAD * HEAD))
        normalizers.append(normalizer.reshape(batch_rows, HEADS * HEAD))
        maxima.append(new_max)
    return (current, jnp.stack(memories), jnp.stack(normalizers), jnp.stack(maxima))
```

```python
import functools

import jax
import jax.numpy as jnp
from jax import lax
from jax.experimental import pallas as pl
from jax.experimental.pallas import tpu as pltpu
from jax.sharding import PartitionSpec as P

HEAD = 64
EPS = 1e-06
BATCH = 4
MESH = pl.DeviceIdType.MESH
F32 = jnp.float32
BF16 = jnp.bfloat16


def dot(a, b):
    return lax.dot_general(a, b, (((1,), (0,)), ((), ())), preferred_element_type=F32)


def lane_iota(shape):
    return lax.broadcasted_iota(jnp.int32, shape, 1)


def kernel(
    n,
    layers,
    tok_h,
    gain_h,
    qw_h,
    kw_h,
    vw_h,
    ow_h,
    ig_h,
    fg_h,
    fb_h,
    pw_h,
    mem_h,
    nrm_h,
    mx_h,
    tok_o,
    mem_o,
    nrm_o,
    mx_o,
    gain,
    w,
    gate_in,
    gate_w,
    fb,
    pw,
    mem,
    mem_t,
    nrm,
    mx,
    old_max,
    bias,
    spread,
    xall,
    psend,
    precv,
    mixall,
    osend,
    orecv,
    load_sem,
    x_sem,
    p_sem,
    m_sem,
    o_sem,
    send_sem,
):
    tp = lax.axis_index("tp")
    dp = lax.axis_index("dp")
    rows, width = tok_h.shape
    heads = width // HEAD
    pairs = width // 128
    tiles = HEAD * HEAD // 128
    cols = 4 * width

    def tp_peer(i):
        return lax.rem(tp + i, n)

    def dp_peer(i):
        return lax.rem(dp + i, n)

    def by_distance(i):
        half = lax.div(i + 1, 2)
        return lax.rem(tp + n + half * (2 * lax.rem(i, 2) - 1), n)

    barrier = pltpu.get_barrier_semaphore()

    def greet(i, carry):
        pl.semaphore_signal(barrier, inc=1, device_id={"tp": tp_peer(i)}, device_id_type=MESH)
        pl.semaphore_signal(barrier, inc=1, device_id={"dp": dp_peer(i)}, device_id_type=MESH)
        return carry

    lax.fori_loop(1, n, greet, 0)

    loads = [
        pltpu.make_async_copy(tok_h, xall.at[0, tp], load_sem.at[0]),
        pltpu.make_async_copy(gain_h, gain, load_sem.at[1]),
        pltpu.make_async_copy(ig_h, gate_in.at[0], load_sem.at[2]),
        pltpu.make_async_copy(fg_h, gate_in.at[1], load_sem.at[3]),
        pltpu.make_async_copy(fb_h, fb, load_sem.at[4]),
        pltpu.make_async_copy(mx_h, mx, load_sem.at[5]),
        pltpu.make_async_copy(nrm_h, nrm, load_sem.at[6]),
    ]
    for i, ref in enumerate((qw_h, kw_h, vw_h, ow_h)):
        loads.append(pltpu.make_async_copy(ref, w.at[i], load_sem.at[7 + i]))
    loads.append(pltpu.make_async_copy(mem_h, mem, load_sem.at[11]))
    loads.append(pltpu.make_async_copy(pw_h, pw, load_sem.at[12]))
    for copy in loads:
        copy.start()

    for c in range(HEAD * HEAD // 512):
        shape = (HEAD, 512)
        block = lane_iota(shape) + c * 512
        row = lax.broadcasted_iota(jnp.int32, shape, 0)
        hit = (block >= row * HEAD) & (block < row * HEAD + HEAD)
        spread[:, c * 512 : (c + 1) * 512] = jnp.where(hit, 1.0, 0.0).astype(BF16)
    for copy in loads[1:7]:
        copy.wait()
    lane = lane_iota((rows, 128))
    row8 = lax.broadcasted_iota(jnp.int32, (rows, 128), 0)
    low = lane < HEAD

    def per_head(values):
        wide = [jnp.broadcast_to(v, (rows, 128)) for v in values]
        return jnp.concatenate(
            [jnp.where(low, wide[2 * p], wide[2 * p + 1]) for p in range(pairs)], axis=1
        )

    def both_halves(x, h):
        part = x[:, (h // 2) * 128 : (h // 2 + 1) * 128]
        turned = pltpu.roll(part, HEAD, 1)
        return jnp.where(low, part, turned) if h % 2 == 0 else jnp.where(low, turned, part)

    eye = (lane_iota((rows, rows)) == lax.broadcasted_iota(jnp.int32, (rows, rows), 0))
    for l in range(layers):
        gate_w[l] = jnp.concatenate(
            [
                gate_in[0, l].astype(F32),
                gate_in[1, l].astype(F32),
                jnp.zeros((128 - 2 * heads, width), F32),
            ],
            axis=0,
        ).astype(BF16)
        old = mx[l]
        old_max[l] = per_head(
            [
                jnp.sum(
                    jnp.where(eye, jnp.broadcast_to(old[h : h + 1, :], (rows, rows)), 0.0),
                    axis=1,
                    keepdims=True,
                )
                for h in range(heads)
            ]
        )
        bias[l] = per_head(
            [jnp.broadcast_to(fb[l : l + 1, h : h + 1], (rows, 1)) for h in range(heads)]
        )

    with jax.named_scope("barrier"):
        pl.semaphore_wait(barrier, 2 * (n - 1))
        loads[0].wait()

    def send_rows(l):
        def far_first(k, carry):
            t = by_distance(n - k)
            pltpu.make_async_remote_copy(
                src_ref=xall.at[l, tp],
                dst_ref=xall.at[l, tp],
                send_sem=send_sem.at[l, 0],
                recv_sem=x_sem.at[l, tp],
                device_id={"tp": t},
                device_id_type=MESH,
            ).start()
            return carry

        lax.fori_loop(1, n, far_first, 0)

    send_rows(0)
    for copy in loads[7:]:
        copy.wait()

    for l in range(layers):

        def turn(r, carry):
            mem_t[l, r] = mem[l, pl.ds(r, rows, stride=heads * tiles), :]
            return carry

        lax.fori_loop(0, heads * tiles, turn, 0, unroll=8)

    for l in range(layers):
        gain_row = gain[l : l + 1, :]

        def project(k, carry):
            sources = [by_distance(k * BATCH + j) for j in range(BATCH)]
            for j, t in enumerate(sources):

                @pl.when(t != tp)
                def _(t=t):
                    with jax.named_scope(f"wait_x{l}"):
                        here = xall.at[l, t]
                        pltpu.make_async_copy(here, here, x_sem.at[l, t]).wait()

            x = jnp.concatenate([xall[l, t].astype(F32) for t in sources], axis=0)
            scaled = (x * gain_row).astype(BF16)
            square = jnp.sum(x * x, axis=1, keepdims=True)
            gates = lax.dot_general(
                scaled, gate_w[l], (((1,), (1,)), ((), ())), preferred_element_type=F32
            )
            lanes = lane_iota(gates.shape)
            gates = jnp.where(lanes == 2 * heads, jnp.broadcast_to(square, gates.shape), gates)
            upper = gates.astype(BF16).astype(F32)
            rest = pltpu.roll(gates - upper, 16, 1)
            parts = [dot(scaled, w[q, l]) for q in range(4)]
            parts.append(jnp.where(lanes < 16, upper, rest))
            for j, t in enumerate(sources):
                block = jnp.concatenate([p[j * rows : (j + 1) * rows] for p in parts], axis=1)
                psend[l, t] = block.astype(BF16)
            for t in sources:

                @pl.when(t == dp)
                def _(t=t):
                    precv[l, dp] = psend[l, t]

                @pl.when(t != dp)
                def _(t=t):
                    pltpu.make_async_remote_copy(
                        src_ref=psend.at[l, t],
                        dst_ref=precv.at[l, dp],
                        send_sem=send_sem.at[l, 1],
                        recv_sem=p_sem.at[l],
                        device_id={"dp": t},
                        device_id_type=MESH,
                    ).start()

            return carry

        lax.fori_loop(0, n // BATCH, project, 0)

        some = precv.at[l, pl.ds(0, n - 1)]
        with jax.named_scope(f"wait_p{l}"):
            pltpu.make_async_copy(some, some, p_sem.at[l]).wait()
        total = precv[l, 0].astype(F32)
        for s in range(1, n):
            total = total + precv[l, s].astype(F32)
        gates = total[:, cols:]
        gates = gates + pltpu.roll(gates, 128 - 16, 1)
        inv_rms = lax.rsqrt(gates[:, 2 * heads : 2 * heads + 1] / (width * n) + EPS)
        gates = gates * inv_rms
        stored = (total[:, :cols] * inv_rms).astype(BF16).astype(F32)
        query = stored[:, :width]
        keys = stored[:, width : 2 * width] * HEAD**-0.5
        values = stored[:, 2 * width : 3 * width]
        outgate = stored[:, 3 * width :]

        def stack(x):
            return jnp.concatenate(
                [x[:, h * HEAD : (h + 1) * HEAD] for h in range(heads)], axis=0
            ).astype(BF16)

        query_rows = stack(query)
        acc = [None] * heads
        chunk = 4
        for c in range(tiles // chunk):
            wide = dot(query_rows, spread[:, c * chunk * 128 : (c + 1) * chunk * 128])
            for j in range(chunk):
                for h in range(heads):
                    term = (
                        wide[h * rows : (h + 1) * rows, j * 128 : (j + 1) * 128]
                        * mem_t[l, (c * chunk + j) * heads + h]
                    )
                    acc[h] = term if acc[h] is None else acc[h] + term

        input_pre = per_head([gates[:, h : h + 1] for h in range(heads)])
        forget_pre = per_head([gates[:, heads + h : heads + h + 1] for h in range(heads)]) + bias[l]
        log_forget = jnp.minimum(forget_pre, 0.0) - jnp.log1p(jnp.exp(-jnp.abs(forget_pre)))
        carried = log_forget + old_max[l]
        new_max = jnp.maximum(carried, input_pre)
        keep = jnp.exp(carried - new_max)
        admit = jnp.exp(input_pre - new_max)
        normalizer = keep * nrm[l] + admit * keys

        def head_sum(x):
            return per_head(
                [
                    jnp.sum(x[:, h * HEAD : (h + 1) * HEAD], axis=1, keepdims=True)
                    for h in range(heads)
                ]
            )

        query_key = head_sum(query * keys)
        denominator = head_sum(query * normalizer)
        folded = [a + pltpu.roll(a, HEAD, 1) for a in acc]
        from_memory = jnp.concatenate(
            [jnp.where(low, folded[2 * p], folded[2 * p + 1]) for p in range(pairs)], axis=1
        )
        numerator = keep * from_memory + admit * query_key * values
        readout = numerator / jnp.maximum(jnp.abs(denominator), jnp.exp(-new_max))
        mixall[l, dp] = (readout * jax.nn.sigmoid(outgate)).astype(BF16)

        def send_mixed(i, carry):
            pltpu.make_async_remote_copy(
                src_ref=mixall.at[l, dp],
                dst_ref=mixall.at[l, dp],
                send_sem=send_sem.at[l, 2],
                recv_sem=m_sem.at[l, dp],
                device_id={"dp": dp_peer(i)},
                device_id_type=MESH,
            ).start()
            return carry

        with jax.named_scope(f"send_m{l}"):
            lax.fori_loop(1, n, send_mixed, 0)

        nrm_o[l] = normalizer
        key_rows = stack(keys)
        keep_h = [both_halves(keep, h) for h in range(heads)]
        value_h = [both_halves(admit * values, h) for h in range(heads)]
        for h in range(heads):
            peak = jnp.where(lane == row8, both_halves(new_max, h), 0.0)
            mx_o[l, h : h + 1, :] = jnp.sum(peak, axis=0, keepdims=True)[:, :rows]
        for c in range(tiles // chunk):
            wide = dot(key_rows, spread[:, c * chunk * 128 : (c + 1) * chunk * 128])
            for j in range(chunk):
                for h in range(heads):
                    r = (c * chunk + j) * heads + h
                    spread_key = wide[h * rows : (h + 1) * rows, j * 128 : (j + 1) * 128]
                    mem_o[l, pl.ds(r, rows, stride=heads * tiles), :] = (
                        keep_h[h] * mem_t[l, r] + spread_key * value_h[h]
                    )

        def leave(k, carry):
            homes = [by_distance(k * BATCH + j) for j in range(BATCH)]
            for t in homes:

                @pl.when(t != dp)
                def _(t=t):
                    with jax.named_scope(f"wait_m{l}"):
                        here = mixall.at[l, t]
                        pltpu.make_async_copy(here, here, m_sem.at[l, t]).wait()

            mixed = jnp.concatenate([mixall[l, t].astype(F32) for t in homes], axis=0)
            part = dot(mixed.astype(BF16), pw[l])
            for j, t in enumerate(homes):
                osend[l, t] = part[j * rows : (j + 1) * rows].astype(BF16)
            for t in homes:

                @pl.when(t == tp)
                def _(t=t):
                    orecv[l, tp] = osend[l, t]

                @pl.when(t != tp)
                def _(t=t):
                    pltpu.make_async_remote_copy(
                        src_ref=osend.at[l, t],
                        dst_ref=orecv.at[l, tp],
                        send_sem=send_sem.at[l, 3],
                        recv_sem=o_sem.at[l],
                        device_id={"tp": t},
                        device_id_type=MESH,
                    ).start()

            return carry

        lax.fori_loop(0, n // BATCH, leave, 0)

        some = orecv.at[l, pl.ds(0, n - 1)]
        with jax.named_scope(f"wait_o{l}"):
            pltpu.make_async_copy(some, some, o_sem.at[l]).wait()
        total = orecv[l, 0].astype(F32)
        for s in range(1, n):
            total = total + orecv[l, s].astype(F32)
        rows_out = (xall[l, tp].astype(F32) + total).astype(BF16)
        if l + 1 < layers:
            xall[l + 1, tp] = rows_out
            send_rows(l + 1)
        else:
            tok_o[...] = rows_out

    for l in range(layers):
        for k, buffer in enumerate((xall, psend, mixall, osend)):
            some = buffer.at[l, pl.ds(0, n - 1)]
            pltpu.make_async_copy(some, some, send_sem.at[l, k]).wait()


def put_out(*refs):
    sems = refs[8]
    copies = [pltpu.make_async_copy(refs[i], refs[4 + i], sems.at[i]) for i in range(4)]
    for copy in copies:
        copy.start()
    for copy in copies:
        copy.wait()


def per_device(
    n,
    tokens,
    norm_gain,
    query_weight,
    key_weight,
    value_weight,
    outgate_weight,
    input_gate_weight,
    forget_gate_weight,
    forget_bias,
    out_weight,
    memory_state,
    normalizer_state,
    maximum_state,
):
    rows, width = tokens.shape
    layers = norm_gain.shape[0]
    heads = width // HEAD
    tiles = HEAD * HEAD // 128
    vmem = pltpu.VMEM

    memory = memory_state.reshape(layers, rows, heads, tiles, 128).transpose(0, 1, 3, 2, 4)
    memory = memory.reshape(layers, rows * tiles * heads, 128)

    in_hbm = pl.BlockSpec(memory_space=pltpu.HBM)
    in_vmem = pl.BlockSpec(memory_space=pltpu.VMEM)
    block = 4 * width + 128
    tokens_out, memory, normalizer, maximum = pl.pallas_call(
        functools.partial(kernel, n, layers),
        out_shape=(
            pltpu.VMEM((rows, width), BF16),
            pltpu.VMEM(memory.shape, F32),
            pltpu.VMEM((layers, rows, width), F32),
            pltpu.VMEM((layers, heads, rows), F32),
        ),
        in_specs=[in_hbm] * 13,
        out_specs=(in_vmem,) * 4,
        scratch_shapes=[
            vmem((layers, width), F32),
            vmem((4, layers, width, width), BF16),
            vmem((2, layers, heads, width), BF16),
            vmem((layers, 128, width), BF16),
            vmem((layers, heads), F32),
            vmem((layers, width, width), BF16),
            vmem(memory.shape, F32),
            vmem((layers, heads * tiles, rows, 128), F32),
            vmem((layers, rows, width), F32),
            vmem((layers, heads, rows), F32),
            vmem((layers, rows, width), F32),
            vmem((layers, rows, width), F32),
            vmem((HEAD, HEAD * HEAD), BF16),
            vmem((layers, n, rows, width), BF16),
            vmem((layers, n, rows, block), BF16),
            vmem((layers, n, rows, block), BF16),
            vmem((layers, n, rows, width), BF16),
            vmem((layers, n, rows, width), BF16),
            vmem((layers, n, rows, width), BF16),
            pltpu.SemaphoreType.DMA((13,)),
            pltpu.SemaphoreType.DMA((layers, n)),
            pltpu.SemaphoreType.DMA((layers,)),
            pltpu.SemaphoreType.DMA((layers, n)),
            pltpu.SemaphoreType.DMA((layers,)),
            pltpu.SemaphoreType.DMA((layers, 4)),
        ],
        compiler_params=pltpu.CompilerParams(
            collective_id=0, has_side_effects=True, vmem_limit_bytes=48 * 1024 * 1024
        ),
        name="cells",
    )(
        *(
            pltpu.with_memory_space_constraint(a, pltpu.HBM)
            for a in (
                tokens,
                norm_gain,
                query_weight,
                key_weight,
                value_weight,
                outgate_weight,
                jnp.swapaxes(input_gate_weight, 1, 2),
                jnp.swapaxes(forget_gate_weight, 1, 2),
                forget_bias,
                out_weight,
                memory,
                normalizer_state,
                jnp.swapaxes(maximum_state, 1, 2),
            )
        )
    )
    results = (tokens_out, memory, normalizer, maximum)
    tokens_out, memory, normalizer, maximum = pl.pallas_call(
        put_out,
        out_shape=tuple(jax.ShapeDtypeStruct(r.shape, r.dtype) for r in results),
        in_specs=[in_vmem] * 4,
        out_specs=(in_hbm,) * 4,
        scratch_shapes=[pltpu.SemaphoreType.DMA((4,))],
        compiler_params=pltpu.CompilerParams(vmem_limit_bytes=4 * 1024 * 1024),
        name="put_out",
    )(*results)
    memory = memory.reshape(layers, rows, tiles, heads, 128).transpose(0, 1, 3, 2, 4)
    return (
        tokens_out,
        memory.reshape(layers, rows, heads, HEAD * HEAD),
        normalizer,
        jnp.swapaxes(maximum, 1, 2),
    )


def solution(mesh):
    n = mesh.shape["tp"]
    assert mesh.shape["dp"] == n
    in_specs = (
        P(("grp", "tp"), "dp"),
        P(None, "dp"),
        P(None, "dp", "tp"),
        P(None, "dp", "tp"),
        P(None, "dp", "tp"),
        P(None, "dp", "tp"),
        P(None, "dp", "tp"),
        P(None, "dp", "tp"),
        P(None, "tp"),
        P(None, "tp", "dp"),
        P(None, ("grp", "dp"), "tp", None),
        P(None, ("grp", "dp"), "tp"),
        P(None, ("grp", "dp"), "tp"),
    )
    out_specs = (
        P(("grp", "tp"), "dp"),
        P(None, ("grp", "dp"), "tp", None),
        P(None, ("grp", "dp"), "tp"),
        P(None, ("grp", "dp"), "tp"),
    )
    return jax.shard_map(
        functools.partial(per_device, n),
        mesh=mesh,
        in_specs=in_specs,
        out_specs=out_specs,
        check_vma=False,
    )
```

```python
import functools

import jax
import jax.numpy as jnp
from jax import lax
from jax.experimental import pallas as pl
from jax.experimental.pallas import tpu as pltpu
from jax.sharding import PartitionSpec as P

HEAD = 64
EPS = 1e-06
BATCH = 4
MESH = pl.DeviceIdType.MESH
F32 = jnp.float32
BF16 = jnp.bfloat16


def dot(a, b):
    return lax.dot_general(a, b, (((1,), (0,)), ((), ())), preferred_element_type=F32)


def lane_iota(shape):
    return lax.broadcasted_iota(jnp.int32, shape, 1)


def kernel(
    n,
    layers,
    tok_h,
    gain_h,
    qw_h,
    kw_h,
    vw_h,
    ow_h,
    ig_h,
    fg_h,
    fb_h,
    pw_h,
    mem_h,
    nrm_h,
    mx_h,
    tok_o,
    mem_o,
    nrm_o,
    mx_o,
    gain,
    w,
    gate_in,
    gate_w,
    fb,
    pw,
    mem,
    mem_t,
    nrm,
    mx,
    old_max,
    bias,
    spread,
    xall,
    pfull,
    pother,
    psend,
    precv,
    mixall,
    osend,
    orecv,
    load_sem,
    x_sem,
    c_sem,
    p_sem,
    m_sem,
    o_sem,
    send_sem,
):
    tp = lax.axis_index("tp")
    dp = lax.axis_index("dp")
    rows, width = tok_h.shape
    heads = width // HEAD
    pairs = width // 128
    tiles = HEAD * HEAD // 128
    cols = 4 * width

    def tp_peer(i):
        return lax.rem(tp + i, n)

    def dp_peer(i):
        return lax.rem(dp + i, n)

    def by_distance(i):
        half = lax.div(i + 1, 2)
        return lax.rem(tp + n + half * (2 * lax.rem(i, 2) - 1), n)

    core = lax.rem(dp, 2)
    chip = lax.div(dp, 2)
    sibling = dp + 1 - 2 * core
    odd = lax.rem(tp + core, 2)

    def of_core(k, parity):
        return [
            by_distance(k * BATCH + lax.select(parity == 0, even, uneven))
            for even, uneven in ((0, 1), (3, 2))
        ]

    barrier = pltpu.get_barrier_semaphore()

    def greet(i, carry):
        pl.semaphore_signal(barrier, inc=1, device_id={"tp": tp_peer(i)}, device_id_type=MESH)
        pl.semaphore_signal(barrier, inc=1, device_id={"dp": dp_peer(i)}, device_id_type=MESH)
        return carry

    lax.fori_loop(1, n, greet, 0)

    loads = [
        pltpu.make_async_copy(tok_h, xall.at[0, tp], load_sem.at[0]),
        pltpu.make_async_copy(gain_h, gain, load_sem.at[1]),
        pltpu.make_async_copy(ig_h, gate_in.at[0], load_sem.at[2]),
        pltpu.make_async_copy(fg_h, gate_in.at[1], load_sem.at[3]),
        pltpu.make_async_copy(fb_h, fb, load_sem.at[4]),
        pltpu.make_async_copy(mx_h, mx, load_sem.at[5]),
        pltpu.make_async_copy(nrm_h, nrm, load_sem.at[6]),
    ]
    for i, ref in enumerate((qw_h, kw_h, vw_h, ow_h)):
        loads.append(pltpu.make_async_copy(ref, w.at[i], load_sem.at[7 + i]))
    loads.append(pltpu.make_async_copy(mem_h, mem, load_sem.at[11]))
    loads.append(pltpu.make_async_copy(pw_h, pw, load_sem.at[12]))
    for copy in loads:
        copy.start()

    for c in range(HEAD * HEAD // 512):
        shape = (HEAD, 512)
        block = lane_iota(shape) + c * 512
        row = lax.broadcasted_iota(jnp.int32, shape, 0)
        hit = (block >= row * HEAD) & (block < row * HEAD + HEAD)
        spread[:, c * 512 : (c + 1) * 512] = jnp.where(hit, 1.0, 0.0).astype(BF16)
    for copy in loads[1:7]:
        copy.wait()
    lane = lane_iota((rows, 128))
    row8 = lax.broadcasted_iota(jnp.int32, (rows, 128), 0)
    low = lane < HEAD

    def per_head(values):
        wide = [jnp.broadcast_to(v, (rows, 128)) for v in values]
        return jnp.concatenate(
            [jnp.where(low, wide[2 * p], wide[2 * p + 1]) for p in range(pairs)], axis=1
        )

    def both_halves(x, h):
        part = x[:, (h // 2) * 128 : (h // 2 + 1) * 128]
        turned = pltpu.roll(part, HEAD, 1)
        return jnp.where(low, part, turned) if h % 2 == 0 else jnp.where(low, turned, part)

    eye = (lane_iota((rows, rows)) == lax.broadcasted_iota(jnp.int32, (rows, rows), 0))
    for l in range(layers):
        gate_w[l] = jnp.concatenate(
            [
                gate_in[0, l].astype(F32),
                gate_in[1, l].astype(F32),
                jnp.zeros((128 - 2 * heads, width), F32),
            ],
            axis=0,
        ).astype(BF16)
        old = mx[l]
        old_max[l] = per_head(
            [
                jnp.sum(
                    jnp.where(eye, jnp.broadcast_to(old[h : h + 1, :], (rows, rows)), 0.0),
                    axis=1,
                    keepdims=True,
                )
                for h in range(heads)
            ]
        )
        bias[l] = per_head(
            [jnp.broadcast_to(fb[l : l + 1, h : h + 1], (rows, 1)) for h in range(heads)]
        )

    with jax.named_scope("barrier"):
        pl.semaphore_wait(barrier, 2 * (n - 1))
        loads[0].wait()

    def send_rows(l):
        def far_first(k, carry):
            t = by_distance(n - k)
            pltpu.make_async_remote_copy(
                src_ref=xall.at[l, tp],
                dst_ref=xall.at[l, tp],
                send_sem=send_sem.at[l, 0],
                recv_sem=x_sem.at[l, tp],
                device_id={"tp": t},
                device_id_type=MESH,
            ).start()
            return carry

        lax.fori_loop(1, n, far_first, 0)

    send_rows(0)
    for copy in loads[7:]:
        copy.wait()

    for l in range(layers):

        def turn(r, carry):
            mem_t[l, r] = mem[l, pl.ds(r, rows, stride=heads * tiles), :]
            return carry

        lax.fori_loop(0, heads * tiles, turn, 0, unroll=8)

    for l in range(layers):
        gain_row = gain[l : l + 1, :]

        def project(k):
            sources = [by_distance(k * BATCH + j) for j in range(BATCH)]
            for t in sources:

                @pl.when(t != tp)
                def _(t=t):
                    with jax.named_scope(f"wait_x{l}"):
                        here = xall.at[l, t]
                        pltpu.make_async_copy(here, here, x_sem.at[l, t]).wait()

            x = jnp.concatenate([xall[l, t].astype(F32) for t in sources], axis=0)
            scaled = (x * gain_row).astype(BF16)
            square = jnp.sum(x * x, axis=1, keepdims=True)
            gates = lax.dot_general(
                scaled, gate_w[l], (((1,), (1,)), ((), ())), preferred_element_type=F32
            )
            gates = jnp.where(
                lane_iota(gates.shape) == 2 * heads, jnp.broadcast_to(square, gates.shape), gates
            )
            parts = [dot(scaled, w[q, l]) for q in range(4)] + [gates]
            for j, t in enumerate(sources):
                pfull[l, t] = jnp.concatenate(
                    [p[j * rows : (j + 1) * rows] for p in parts], axis=1
                )
            for t in of_core(k, 1 - odd):
                pltpu.make_async_remote_copy(
                    src_ref=pfull.at[l, t],
                    dst_ref=pother.at[l, t],
                    send_sem=send_sem.at[l, 4],
                    recv_sem=c_sem.at[l, t],
                    device_id={"dp": sibling},
                    device_id_type=MESH,
                ).start()

        def pass_on(k):
            for t in of_core(k, odd):
                with jax.named_scope(f"wait_c{l}"):
                    there = pother.at[l, t]
                    pltpu.make_async_copy(there, there, c_sem.at[l, t]).wait()
                both = pfull[l, t] + pother[l, t]
                gates = both[:, cols:]
                upper = gates.astype(BF16).astype(F32)
                rest = pltpu.roll(gates - upper, 16, 1)
                gates = jnp.where(lane < 16, upper, rest)
                block = jnp.concatenate([both[:, :cols], gates], axis=1)
                psend[l, t] = block.astype(BF16)

                @pl.when(t == dp)
                def _(t=t):
                    precv[l, chip] = psend[l, t]

                @pl.when(t != dp)
                def _(t=t):
                    pltpu.make_async_remote_copy(
                        src_ref=psend.at[l, t],
                        dst_ref=precv.at[l, chip],
                        send_sem=send_sem.at[l, 1],
                        recv_sem=p_sem.at[l],
                        device_id={"dp": t},
                        device_id_type=MESH,
                    ).start()

        for k in range(n // BATCH):
            project(k)
            if k > 0:
                pass_on(k - 1)
        pass_on(n // BATCH - 1)

        some = precv.at[l, pl.ds(0, n // 2 - 1)]
        with jax.named_scope(f"wait_p{l}"):
            pltpu.make_async_copy(some, some, p_sem.at[l]).wait()
        total = precv[l, 0].astype(F32)
        for s in range(1, n // 2):
            total = total + precv[l, s].astype(F32)
        gates = total[:, cols:]
        gates = gates + pltpu.roll(gates, 128 - 16, 1)
        inv_rms = lax.rsqrt(gates[:, 2 * heads : 2 * heads + 1] / (width * n) + EPS)
        gates = gates * inv_rms
        stored = (total[:, :cols] * inv_rms).astype(BF16).astype(F32)
        query = stored[:, :width]
        keys = stored[:, width : 2 * width] * HEAD**-0.5
        values = stored[:, 2 * width : 3 * width]
        outgate = stored[:, 3 * width :]

        def stack(x):
            return jnp.concatenate(
                [x[:, h * HEAD : (h + 1) * HEAD] for h in range(heads)], axis=0
            ).astype(BF16)

        query_rows = stack(query)
        acc = [None] * heads
        chunk = 4
        for c in range(tiles // chunk):
            wide = dot(query_rows, spread[:, c * chunk * 128 : (c + 1) * chunk * 128])
            for j in range(chunk):
                for h in range(heads):
                    term = (
                        wide[h * rows : (h + 1) * rows, j * 128 : (j + 1) * 128]
                        * mem_t[l, (c * chunk + j) * heads + h]
                    )
                    acc[h] = term if acc[h] is None else acc[h] + term

        input_pre = per_head([gates[:, h : h + 1] for h in range(heads)])
        forget_pre = per_head([gates[:, heads + h : heads + h + 1] for h in range(heads)]) + bias[l]
        log_forget = jnp.minimum(forget_pre, 0.0) - jnp.log1p(jnp.exp(-jnp.abs(forget_pre)))
        carried = log_forget + old_max[l]
        new_max = jnp.maximum(carried, input_pre)
        keep = jnp.exp(carried - new_max)
        admit = jnp.exp(input_pre - new_max)
        normalizer = keep * nrm[l] + admit * keys

        def head_sum(x):
            return per_head(
                [
                    jnp.sum(x[:, h * HEAD : (h + 1) * HEAD], axis=1, keepdims=True)
                    for h in range(heads)
                ]
            )

        query_key = head_sum(query * keys)
        denominator = head_sum(query * normalizer)
        folded = [a + pltpu.roll(a, HEAD, 1) for a in acc]
        from_memory = jnp.concatenate(
            [jnp.where(low, folded[2 * p], folded[2 * p + 1]) for p in range(pairs)], axis=1
        )
        numerator = keep * from_memory + admit * query_key * values
        readout = numerator / jnp.maximum(jnp.abs(denominator), jnp.exp(-new_max))
        mixall[l, dp] = (readout * jax.nn.sigmoid(outgate)).astype(BF16)

        def send_mixed(i, carry):
            pltpu.make_async_remote_copy(
                src_ref=mixall.at[l, dp],
                dst_ref=mixall.at[l, dp],
                send_sem=send_sem.at[l, 2],
                recv_sem=m_sem.at[l, dp],
                device_id={"dp": dp_peer(i)},
                device_id_type=MESH,
            ).start()
            return carry

        with jax.named_scope(f"send_m{l}"):
            lax.fori_loop(1, n, send_mixed, 0)

        nrm_o[l] = normalizer
        key_rows = stack(keys)
        keep_h = [both_halves(keep, h) for h in range(heads)]
        value_h = [both_halves(admit * values, h) for h in range(heads)]
        for h in range(heads):
            peak = jnp.where(lane == row8, both_halves(new_max, h), 0.0)
            mx_o[l, h : h + 1, :] = jnp.sum(peak, axis=0, keepdims=True)[:, :rows]
        for c in range(tiles // chunk):
            wide = dot(key_rows, spread[:, c * chunk * 128 : (c + 1) * chunk * 128])
            for j in range(chunk):
                for h in range(heads):
                    r = (c * chunk + j) * heads + h
                    spread_key = wide[h * rows : (h + 1) * rows, j * 128 : (j + 1) * 128]
                    mem_o[l, pl.ds(r, rows, stride=heads * tiles), :] = (
                        keep_h[h] * mem_t[l, r] + spread_key * value_h[h]
                    )

        def leave(k, carry):
            homes = [by_distance(k * BATCH + j) for j in range(BATCH)]
            for t in homes:

                @pl.when(t != dp)
                def _(t=t):
                    with jax.named_scope(f"wait_m{l}"):
                        here = mixall.at[l, t]
                        pltpu.make_async_copy(here, here, m_sem.at[l, t]).wait()

            mixed = jnp.concatenate([mixall[l, t].astype(F32) for t in homes], axis=0)
            part = dot(mixed.astype(BF16), pw[l])
            for j, t in enumerate(homes):
                osend[l, t] = part[j * rows : (j + 1) * rows].astype(BF16)
            for t in homes:

                @pl.when(t == tp)
                def _(t=t):
                    orecv[l, tp] = osend[l, t]

                @pl.when(t != tp)
                def _(t=t):
                    pltpu.make_async_remote_copy(
                        src_ref=osend.at[l, t],
                        dst_ref=orecv.at[l, tp],
                        send_sem=send_sem.at[l, 3],
                        recv_sem=o_sem.at[l],
                        device_id={"tp": t},
                        device_id_type=MESH,
                    ).start()

            return carry

        lax.fori_loop(0, n // BATCH, leave, 0)

        some = orecv.at[l, pl.ds(0, n - 1)]
        with jax.named_scope(f"wait_o{l}"):
            pltpu.make_async_copy(some, some, o_sem.at[l]).wait()
        total = orecv[l, 0].astype(F32)
        for s in range(1, n):
            total = total + orecv[l, s].astype(F32)
        rows_out = (xall[l, tp].astype(F32) + total).astype(BF16)
        if l + 1 < layers:
            xall[l + 1, tp] = rows_out
            send_rows(l + 1)
        else:
            tok_o[...] = rows_out

    for l in range(layers):
        sent = ((xall, n - 1), (psend, n // 2 - 1), (mixall, n - 1), (osend, n - 1), (pfull, n // 2))
        for k, (buffer, count) in enumerate(sent):
            some = buffer.at[l, pl.ds(0, count)]
            pltpu.make_async_copy(some, some, send_sem.at[l, k]).wait()


def put_out(*refs):
    sems = refs[8]
    copies = [pltpu.make_async_copy(refs[i], refs[4 + i], sems.at[i]) for i in range(4)]
    for copy in copies:
        copy.start()
    for copy in copies:
        copy.wait()


def per_device(
    n,
    tokens,
    norm_gain,
    query_weight,
    key_weight,
    value_weight,
    outgate_weight,
    input_gate_weight,
    forget_gate_weight,
    forget_bias,
    out_weight,
    memory_state,
    normalizer_state,
    maximum_state,
):
    rows, width = tokens.shape
    layers = norm_gain.shape[0]
    heads = width // HEAD
    tiles = HEAD * HEAD // 128
    vmem = pltpu.VMEM

    memory = memory_state.reshape(layers, rows, heads, tiles, 128).transpose(0, 1, 3, 2, 4)
    memory = memory.reshape(layers, rows * tiles * heads, 128)

    in_hbm = pl.BlockSpec(memory_space=pltpu.HBM)
    in_vmem = pl.BlockSpec(memory_space=pltpu.VMEM)
    block = 4 * width + 128
    tokens_out, memory, normalizer, maximum = pl.pallas_call(
        functools.partial(kernel, n, layers),
        out_shape=(
            pltpu.VMEM((rows, width), BF16),
            pltpu.VMEM(memory.shape, F32),
            pltpu.VMEM((layers, rows, width), F32),
            pltpu.VMEM((layers, heads, rows), F32),
        ),
        in_specs=[in_hbm] * 13,
        out_specs=(in_vmem,) * 4,
        scratch_shapes=[
            vmem((layers, width), F32),
            vmem((4, layers, width, width), BF16),
            vmem((2, layers, heads, width), BF16),
            vmem((layers, 128, width), BF16),
            vmem((layers, heads), F32),
            vmem((layers, width, width), BF16),
            vmem(memory.shape, F32),
            vmem((layers, heads * tiles, rows, 128), F32),
            vmem((layers, rows, width), F32),
            vmem((layers, heads, rows), F32),
            vmem((layers, rows, width), F32),
            vmem((layers, rows, width), F32),
            vmem((HEAD, HEAD * HEAD), BF16),
            vmem((layers, n, rows, width), BF16),
            vmem((layers, n, rows, block), F32),
            vmem((layers, n, rows, block), F32),
            vmem((layers, n, rows, block), BF16),
            vmem((layers, n // 2, rows, block), BF16),
            vmem((layers, n, rows, width), BF16),
            vmem((layers, n, rows, width), BF16),
            vmem((layers, n, rows, width), BF16),
            pltpu.SemaphoreType.DMA((13,)),
            pltpu.SemaphoreType.DMA((layers, n)),
            pltpu.SemaphoreType.DMA((layers, n)),
            pltpu.SemaphoreType.DMA((layers,)),
            pltpu.SemaphoreType.DMA((layers, n)),
            pltpu.SemaphoreType.DMA((layers,)),
            pltpu.SemaphoreType.DMA((layers, 5)),
        ],
        compiler_params=pltpu.CompilerParams(
            collective_id=0, has_side_effects=True, vmem_limit_bytes=48 * 1024 * 1024
        ),
        name="cells",
    )(
        *(
            pltpu.with_memory_space_constraint(a, pltpu.HBM)
            for a in (
                tokens,
                norm_gain,
                query_weight,
                key_weight,
                value_weight,
                outgate_weight,
                jnp.swapaxes(input_gate_weight, 1, 2),
                jnp.swapaxes(forget_gate_weight, 1, 2),
                forget_bias,
                out_weight,
                memory,
                normalizer_state,
                jnp.swapaxes(maximum_state, 1, 2),
            )
        )
    )
    results = (tokens_out, memory, normalizer, maximum)
    tokens_out, memory, normalizer, maximum = pl.pallas_call(
        put_out,
        out_shape=tuple(jax.ShapeDtypeStruct(r.shape, r.dtype) for r in results),
        in_specs=[in_vmem] * 4,
        out_specs=(in_hbm,) * 4,
        scratch_shapes=[pltpu.SemaphoreType.DMA((4,))],
        compiler_params=pltpu.CompilerParams(vmem_limit_bytes=4 * 1024 * 1024),
        name="put_out",
    )(*results)
    memory = memory.reshape(layers, rows, tiles, heads, 128).transpose(0, 1, 3, 2, 4)
    return (
        tokens_out,
        memory.reshape(layers, rows, heads, HEAD * HEAD),
        normalizer,
        jnp.swapaxes(maximum, 1, 2),
    )


def solution(mesh):
    n = mesh.shape["tp"]
    assert mesh.shape["dp"] == n
    in_specs = (
        P(("grp", "tp"), "dp"),
        P(None, "dp"),
        P(None, "dp", "tp"),
        P(None, "dp", "tp"),
        P(None, "dp", "tp"),
        P(None, "dp", "tp"),
        P(None, "dp", "tp"),
        P(None, "dp", "tp"),
        P(None, "tp"),
        P(None, "tp", "dp"),
        P(None, ("grp", "dp"), "tp", None),
        P(None, ("grp", "dp"), "tp"),
        P(None, ("grp", "dp"), "tp"),
    )
    out_specs = (
        P(("grp", "tp"), "dp"),
        P(None, ("grp", "dp"), "tp", None),
        P(None, ("grp", "dp"), "tp"),
        P(None, ("grp", "dp"), "tp"),
    )
    return jax.shard_map(
        functools.partial(per_device, n),
        mesh=mesh,
        in_specs=in_specs,
        out_specs=out_specs,
        check_vma=False,
    )
```

```python
import functools

import jax
import jax.numpy as jnp
from jax import lax
from jax.experimental import pallas as pl
from jax.experimental.pallas import tpu as pltpu
from jax.sharding import PartitionSpec as P

HEAD = 64
EPS = 1e-06
BATCH = 4
HUB = 1
MESH = pl.DeviceIdType.MESH
F32 = jnp.float32
BF16 = jnp.bfloat16


def dot(a, b):
    return lax.dot_general(a, b, (((1,), (0,)), ((), ())), preferred_element_type=F32)


def lane_iota(shape):
    return lax.broadcasted_iota(jnp.int32, shape, 1)


def kernel(
    n,
    layers,
    tok_h,
    gain_h,
    qw_h,
    kw_h,
    vw_h,
    ow_h,
    ig_h,
    fg_h,
    fb_h,
    pw_h,
    mem_h,
    nrm_h,
    mx_h,
    tok_o,
    mem_o,
    nrm_o,
    mx_o,
    gain,
    w,
    gate_in,
    gate_w,
    fb,
    pw,
    mem,
    mem_t,
    nrm,
    mx,
    old_max,
    bias,
    spread,
    xall,
    pfull,
    pother,
    psend,
    precv,
    mixall,
    osend,
    orecv,
    load_sem,
    x_sem,
    c_sem,
    p_sem,
    m_sem,
    o_sem,
    send_sem,
    hub_sem,
    plane_sem,
    ready_sem,
):
    tp = lax.axis_index("tp")
    dp = lax.axis_index("dp")
    rows, width = tok_h.shape
    heads = width // HEAD
    pairs = width // 128
    tiles = HEAD * HEAD // 128
    cols = 4 * width

    def dp_peer(i):
        return lax.rem(dp + i, n)

    def by_distance(i):
        half = lax.div(i + 1, 2)
        return lax.rem(tp + n + half * (2 * lax.rem(i, 2) - 1), n)

    def arrival(i):
        return lax.select(i < n - 2, HUB + i, lax.select(i == n - 2, 0, n - 1))

    def by_owner(i):
        return lax.rem(by_distance(lax.div(i, 2)) + (n // 2) * lax.rem(i, 2), n)

    opposite = lax.rem(tp + n // 2, n)
    core = lax.rem(dp, 2)
    chip = lax.div(dp, 2)
    sibling = dp + 1 - 2 * core
    odd = lax.rem(tp + core, 2)

    def batch_of(l, k):
        places = range(k * BATCH, (k + 1) * BATCH)
        where = arrival if l == 0 else by_owner
        return [where(i) for i in places]

    def of_core(l, k, mine):
        if l == 0:
            order = [(HUB + i) % 2 if i < n - 2 else (0, 1)[i - n + 2] for i in range(n)]
            flag = core
        else:
            order = [((i // 2 + 1) // 2) % 2 for i in range(n)]
            flag = odd
        places = range(k * BATCH, (k + 1) * BATCH)
        even = [i for i in places if order[i] == 0]
        uneven = [i for i in places if order[i] == 1]
        flag = flag if mine else 1 - flag
        where = arrival if l == 0 else by_owner
        return [where(lax.select(flag == 0, e, u)) for e, u in zip(even, uneven, strict=True)]

    barrier = pltpu.get_barrier_semaphore()
    at_hub = tp == HUB

    @pl.when(at_hub)
    def _():
        def greet(i, carry):
            pl.semaphore_signal(barrier, inc=1, device_id={"dp": dp_peer(i)}, device_id_type=MESH)
            there = {"tp": lax.rem(tp + i, n)}
            pl.semaphore_signal(barrier, inc=1, device_id=there, device_id_type=MESH)
            return carry

        lax.fori_loop(1, n, greet, 0)

    loads = [
        pltpu.make_async_copy(tok_h, xall.at[0, tp], load_sem.at[0]),
        pltpu.make_async_copy(gain_h, gain, load_sem.at[1]),
        pltpu.make_async_copy(ig_h, gate_in.at[0], load_sem.at[2]),
        pltpu.make_async_copy(fg_h, gate_in.at[1], load_sem.at[3]),
        pltpu.make_async_copy(fb_h, fb, load_sem.at[4]),
        pltpu.make_async_copy(mx_h, mx, load_sem.at[5]),
        pltpu.make_async_copy(nrm_h, nrm, load_sem.at[6]),
    ]
    for i, ref in enumerate((qw_h, kw_h, vw_h, ow_h)):
        loads.append(pltpu.make_async_copy(ref, w.at[i], load_sem.at[7 + i]))
    loads.append(pltpu.make_async_copy(mem_h, mem, load_sem.at[11]))
    loads.append(pltpu.make_async_copy(pw_h, pw, load_sem.at[12]))
    for copy in loads:
        copy.start()

    with jax.named_scope("barrier"):
        pl.semaphore_wait(barrier, lax.select(at_hub, n - 1, 1))
        loads[0].wait()

    def row_copy(l, block, t, sem):
        return pltpu.make_async_remote_copy(
            src_ref=xall.at[l, block],
            dst_ref=xall.at[l, block],
            send_sem=sem,
            recv_sem=x_sem.at[l, block],
            device_id={"tp": t},
            device_id_type=MESH,
        )

    def wait_rows(l, block):
        with jax.named_scope(f"wait_x{l}"):
            here = xall.at[l, block]
            pltpu.make_async_copy(here, here, x_sem.at[l, block]).wait()

    def send_rows(l):
        def far_first(k, carry):
            t = by_distance(n // 2 - k)
            row_copy(l, tp, t, send_sem.at[l, 0]).start()
            row_copy(l, opposite, t, send_sem.at[l, 0]).start()
            return carry

        lax.fori_loop(1, n // 2, far_first, 0)

    @pl.when(jnp.logical_not(at_hub))
    def _():
        row_copy(0, tp, HUB, send_sem.at[0, 0]).start()

    for c in range(HEAD * HEAD // 512):
        shape = (HEAD, 512)
        block = lane_iota(shape) + c * 512
        row = lax.broadcasted_iota(jnp.int32, shape, 0)
        hit = (block >= row * HEAD) & (block < row * HEAD + HEAD)
        spread[:, c * 512 : (c + 1) * 512] = jnp.where(hit, 1.0, 0.0).astype(BF16)
    for copy in loads[1:7]:
        copy.wait()
    lane = lane_iota((rows, 128))
    row8 = lax.broadcasted_iota(jnp.int32, (rows, 128), 0)
    low = lane < HEAD

    def per_head(values):
        wide = [jnp.broadcast_to(v, (rows, 128)) for v in values]
        return jnp.concatenate(
            [jnp.where(low, wide[2 * p], wide[2 * p + 1]) for p in range(pairs)], axis=1
        )

    def both_halves(x, h):
        part = x[:, (h // 2) * 128 : (h // 2 + 1) * 128]
        turned = pltpu.roll(part, HEAD, 1)
        return jnp.where(low, part, turned) if h % 2 == 0 else jnp.where(low, turned, part)

    eye = (lane_iota((rows, rows)) == lax.broadcasted_iota(jnp.int32, (rows, rows), 0))
    for l in range(layers):
        gate_w[l] = jnp.concatenate(
            [
                gate_in[0, l].astype(F32),
                gate_in[1, l].astype(F32),
                jnp.zeros((128 - 2 * heads, width), F32),
            ],
            axis=0,
        ).astype(BF16)
        old = mx[l]
        old_max[l] = per_head(
            [
                jnp.sum(
                    jnp.where(eye, jnp.broadcast_to(old[h : h + 1, :], (rows, rows)), 0.0),
                    axis=1,
                    keepdims=True,
                )
                for h in range(heads)
            ]
        )
        bias[l] = per_head(
            [jnp.broadcast_to(fb[l : l + 1, h : h + 1], (rows, 1)) for h in range(heads)]
        )

    for copy in loads[7:12]:
        copy.wait()

    for l in range(layers):

        def turn(r, carry):
            mem_t[l, r] = mem[l, pl.ds(r, rows, stride=heads * tiles), :]
            return carry

        lax.fori_loop(0, heads * tiles, turn, 0, unroll=8)

    @pl.when(at_hub)
    def _():
        def relay(j, carry):
            block = arrival(j + 1)
            wait_rows(0, block)

            def tell(i, c):
                there = {"dp": dp_peer(i)}
                pl.semaphore_signal(
                    plane_sem.at[block], inc=1, device_id=there, device_id_type=MESH
                )
                return c

            lax.fori_loop(1, n, tell, 0)

            def to_known(q, c):
                t = arrival(q)
                row_copy(0, block, t, hub_sem.at[t]).start()
                return c

            lax.fori_loop(1, j + 1, to_known, 0)

            def catch_up(q, c):
                row_copy(0, arrival(q), block, hub_sem.at[block]).start()
                return c

            lax.fori_loop(0, j + 1, catch_up, 0)

            @pl.when(j > 0)
            def _():
                settle(j - 1)

            return carry

        def settle(j):
            t = arrival(j + 1)
            pl.semaphore_wait(plane_sem.at[t], n - 1)
            pl.semaphore_signal(ready_sem, inc=1, device_id={"tp": t}, device_id_type=MESH)

        lax.fori_loop(0, n - 1, relay, 0)
        settle(n - 2)

    loads[12].wait()

    for l in range(layers):
        gain_row = gain[l : l + 1, :]

        def project(k):
            sources = batch_of(l, k)
            for t in sources:
                @pl.when((t != tp) & (jnp.logical_not(at_hub) if l == 0 else t != opposite))
                def _(t=t):
                    wait_rows(l, t)

            x = jnp.concatenate([xall[l, t].astype(F32) for t in sources], axis=0)
            scaled = (x * gain_row).astype(BF16)
            square = jnp.sum(x * x, axis=1, keepdims=True)
            gates = lax.dot_general(
                scaled, gate_w[l], (((1,), (1,)), ((), ())), preferred_element_type=F32
            )
            gates = jnp.where(
                lane_iota(gates.shape) == 2 * heads, jnp.broadcast_to(square, gates.shape), gates
            )
            parts = [dot(scaled, w[q, l]) for q in range(4)] + [gates]
            for j, t in enumerate(sources):
                pfull[l, t] = jnp.concatenate(
                    [p[j * rows : (j + 1) * rows] for p in parts], axis=1
                )
        def give(k):
            for t in of_core(l, k, False):
                pltpu.make_async_remote_copy(
                    src_ref=pfull.at[l, t],
                    dst_ref=pother.at[l, t],
                    send_sem=send_sem.at[l, 4],
                    recv_sem=c_sem.at[l, t],
                    device_id={"dp": sibling},
                    device_id_type=MESH,
                ).start()

        def pass_on(k):
            for t in of_core(l, k, True):
                with jax.named_scope(f"wait_c{l}"):
                    there = pother.at[l, t]
                    pltpu.make_async_copy(there, there, c_sem.at[l, t]).wait()
                both = pfull[l, t] + pother[l, t]
                gates = both[:, cols:]
                upper = gates.astype(BF16).astype(F32)
                rest = pltpu.roll(gates - upper, 16, 1)
                gates = jnp.where(lane < 16, upper, rest)
                block = jnp.concatenate([both[:, :cols], gates], axis=1)
                psend[l, t] = block.astype(BF16)

                @pl.when(t == dp)
                def _(t=t):
                    precv[l, chip] = psend[l, t]

                @pl.when(t != dp)
                def _(t=t):
                    pltpu.make_async_remote_copy(
                        src_ref=psend.at[l, t],
                        dst_ref=precv.at[l, chip],
                        send_sem=send_sem.at[l, 1],
                        recv_sem=p_sem.at[l],
                        device_id={"dp": t},
                        device_id_type=MESH,
                    ).start()

        last = n // BATCH - 1
        if l == 0:
            for k in range(last):
                project(k)

            @pl.when(jnp.logical_not(at_hub))
            def _():
                with jax.named_scope("ready"):
                    pl.semaphore_wait(ready_sem, 1)

            for k in range(last):
                give(k)
            for k in range(last):
                pass_on(k)
            project(last)
            give(last)
        else:
            for k in range(last + 1):
                project(k)
                give(k)
                if k > 0:
                    pass_on(k - 1)
        pass_on(last)

        some = precv.at[l, pl.ds(0, n // 2 - 1)]
        with jax.named_scope(f"wait_p{l}"):
            pltpu.make_async_copy(some, some, p_sem.at[l]).wait()
        total = precv[l, 0].astype(F32)
        for s in range(1, n // 2):
            total = total + precv[l, s].astype(F32)
        gates = total[:, cols:]
        gates = gates + pltpu.roll(gates, 128 - 16, 1)
        inv_rms = lax.rsqrt(gates[:, 2 * heads : 2 * heads + 1] / (width * n) + EPS)
        gates = gates * inv_rms
        stored = (total[:, :cols] * inv_rms).astype(BF16).astype(F32)
        query = stored[:, :width]
        keys = stored[:, width : 2 * width] * HEAD**-0.5
        values = stored[:, 2 * width : 3 * width]
        outgate = stored[:, 3 * width :]

        def stack(x):
            return jnp.concatenate(
                [x[:, h * HEAD : (h + 1) * HEAD] for h in range(heads)], axis=0
            ).astype(BF16)

        query_rows = stack(query)
        acc = [None] * heads
        chunk = 4
        for c in range(tiles // chunk):
            wide = dot(query_rows, spread[:, c * chunk * 128 : (c + 1) * chunk * 128])
            for j in range(chunk):
                for h in range(heads):
                    term = (
                        wide[h * rows : (h + 1) * rows, j * 128 : (j + 1) * 128]
                        * mem_t[l, (c * chunk + j) * heads + h]
                    )
                    acc[h] = term if acc[h] is None else acc[h] + term

        input_pre = per_head([gates[:, h : h + 1] for h in range(heads)])
        forget_pre = per_head([gates[:, heads + h : heads + h + 1] for h in range(heads)]) + bias[l]
        log_forget = jnp.minimum(forget_pre, 0.0) - jnp.log1p(jnp.exp(-jnp.abs(forget_pre)))
        carried = log_forget + old_max[l]
        new_max = jnp.maximum(carried, input_pre)
        keep = jnp.exp(carried - new_max)
        admit = jnp.exp(input_pre - new_max)
        normalizer = keep * nrm[l] + admit * keys

        def head_sum(x):
            return per_head(
                [
                    jnp.sum(x[:, h * HEAD : (h + 1) * HEAD], axis=1, keepdims=True)
                    for h in range(heads)
                ]
            )

        query_key = head_sum(query * keys)
        denominator = head_sum(query * normalizer)
        folded = [a + pltpu.roll(a, HEAD, 1) for a in acc]
        from_memory = jnp.concatenate(
            [jnp.where(low, folded[2 * p], folded[2 * p + 1]) for p in range(pairs)], axis=1
        )
        numerator = keep * from_memory + admit * query_key * values
        readout = numerator / jnp.maximum(jnp.abs(denominator), jnp.exp(-new_max))
        mixall[l, dp] = (readout * jax.nn.sigmoid(outgate)).astype(BF16)

        def send_mixed(k, carry):
            half = lax.div(k, 2)
            i = lax.select(lax.rem(k, 2) == 0, n // 2 - half, n // 2 + half)
            pltpu.make_async_remote_copy(
                src_ref=mixall.at[l, dp],
                dst_ref=mixall.at[l, dp],
                send_sem=send_sem.at[l, 2],
                recv_sem=m_sem.at[l, dp],
                device_id={"dp": dp_peer(i)},
                device_id_type=MESH,
            ).start()
            return carry

        with jax.named_scope(f"send_m{l}"):
            lax.fori_loop(1, n, send_mixed, 0)

        nrm_o[l] = normalizer
        key_rows = stack(keys)
        keep_h = [both_halves(keep, h) for h in range(heads)]
        value_h = [both_halves(admit * values, h) for h in range(heads)]
        for h in range(heads):
            peak = jnp.where(lane == row8, both_halves(new_max, h), 0.0)
            mx_o[l, h : h + 1, :] = jnp.sum(peak, axis=0, keepdims=True)[:, :rows]
        for c in range(tiles // chunk):
            wide = dot(key_rows, spread[:, c * chunk * 128 : (c + 1) * chunk * 128])
            for j in range(chunk):
                for h in range(heads):
                    r = (c * chunk + j) * heads + h
                    spread_key = wide[h * rows : (h + 1) * rows, j * 128 : (j + 1) * 128]
                    mem_o[l, pl.ds(r, rows, stride=heads * tiles), :] = (
                        keep_h[h] * mem_t[l, r] + spread_key * value_h[h]
                    )

        owners = 2 if l + 1 < layers else 1

        def leave(k, carry):
            homes = [by_distance(k * BATCH + j) for j in range(BATCH)]
            if l == 0:
                homes = [
                    lax.select(tp == n - 1, by_distance(n - 1 - i), arrival(i))
                    for i in (k * BATCH + j for j in range(BATCH))
                ]
            for t in homes:

                @pl.when(t != dp)
                def _(t=t):
                    with jax.named_scope(f"wait_m{l}"):
                        here = mixall.at[l, t]
                        pltpu.make_async_copy(here, here, m_sem.at[l, t]).wait()

            mixed = jnp.concatenate([mixall[l, t].astype(F32) for t in homes], axis=0)
            part = dot(mixed.astype(BF16), pw[l])
            for j, t in enumerate(homes):
                osend[l, t] = part[j * rows : (j + 1) * rows].astype(BF16)
            for t in reversed(homes):

                for owner in range(owners):
                    home = lax.rem(t + owner * (n // 2), n)

                    @pl.when(home == tp)
                    def _(t=t, owner=owner):
                        orecv[l, owner, tp] = osend[l, t]

                    @pl.when(home != tp)
                    def _(t=t, owner=owner, home=home):
                        pltpu.make_async_remote_copy(
                            src_ref=osend.at[l, t],
                            dst_ref=orecv.at[l, owner, tp],
                            send_sem=send_sem.at[l, 3 + 2 * owner],
                            recv_sem=o_sem.at[l, owner],
                            device_id={"tp": home},
                            device_id_type=MESH,
                        ).start()

            return carry

        lax.fori_loop(0, n // BATCH, leave, 0)

        for owner in range(owners):
            some = orecv.at[l, owner, pl.ds(0, n - 1)]
            with jax.named_scope(f"wait_o{l}"):
                pltpu.make_async_copy(some, some, o_sem.at[l, owner]).wait()
        for owner in range(owners):
            home = (tp, opposite)[owner]
            total = orecv[l, owner, 0].astype(F32)
            for s in range(1, n):
                total = total + orecv[l, owner, s].astype(F32)
            rows_out = (xall[l, home].astype(F32) + total).astype(BF16)
            if l + 1 < layers:
                xall[l + 1, home] = rows_out
            else:
                tok_o[...] = rows_out
        if l + 1 < layers:
            send_rows(l + 1)

    for l in range(layers):
        sent = [(xall, n - 2), (psend, n // 2 - 1), (mixall, n - 1), (osend, n - 1), (pfull, n // 2)]
        if l + 1 < layers:
            sent.append((osend, n - 1))
        for k, (buffer, count) in enumerate(sent):
            some = buffer.at[l, pl.ds(0, count)]
            if l > 0 or k > 0:
                pltpu.make_async_copy(some, some, send_sem.at[l, k]).wait()

    @pl.when(jnp.logical_not(at_hub))
    def _():
        row_copy(0, tp, HUB, send_sem.at[0, 0]).wait_send()

    @pl.when(at_hub)
    def _():
        def handed_on(j, carry):
            some = xall.at[0, pl.ds(0, n - 1)]
            pltpu.make_async_copy(some, some, hub_sem.at[arrival(j + 1)]).wait()
            return carry

        lax.fori_loop(0, n - 1, handed_on, 0)


def put_out(*refs):
    sems = refs[8]
    pieces = 8
    copies = []
    for src, dst in zip(refs[:4], refs[4:8], strict=True):
        if src.ndim < 3 or src.shape[1] < 1024:
            copies.append((src, dst))
            continue
        step = src.shape[1] * src.shape[0] // pieces
        for at in range(0, src.shape[1], step):
            for l in range(src.shape[0]):
                copies.append((src.at[l, at : at + step], dst.at[l, at : at + step]))
    copies = [pltpu.make_async_copy(*c, sems.at[i]) for i, c in enumerate(copies)]
    for copy in copies:
        copy.start()
    for copy in copies:
        copy.wait()


def per_device(
    n,
    tokens,
    norm_gain,
    query_weight,
    key_weight,
    value_weight,
    outgate_weight,
    input_gate_weight,
    forget_gate_weight,
    forget_bias,
    out_weight,
    memory_state,
    normalizer_state,
    maximum_state,
):
    rows, width = tokens.shape
    layers = norm_gain.shape[0]
    heads = width // HEAD
    tiles = HEAD * HEAD // 128
    vmem = pltpu.VMEM

    memory = memory_state.reshape(layers, rows, heads, tiles, 128).transpose(0, 1, 3, 2, 4)
    memory = memory.reshape(layers, rows * tiles * heads, 128)

    in_hbm = pl.BlockSpec(memory_space=pltpu.HBM)
    in_vmem = pl.BlockSpec(memory_space=pltpu.VMEM)
    block = 4 * width + 128
    tokens_out, memory, normalizer, maximum = pl.pallas_call(
        functools.partial(kernel, n, layers),
        out_shape=(
            pltpu.VMEM((rows, width), BF16),
            pltpu.VMEM(memory.shape, F32),
            pltpu.VMEM((layers, rows, width), F32),
            pltpu.VMEM((layers, heads, rows), F32),
        ),
        in_specs=[in_hbm] * 13,
        out_specs=(in_vmem,) * 4,
        scratch_shapes=[
            vmem((layers, width), F32),
            vmem((4, layers, width, width), BF16),
            vmem((2, layers, heads, width), BF16),
            vmem((layers, 128, width), BF16),
            vmem((layers, heads), F32),
            vmem((layers, width, width), BF16),
            vmem(memory.shape, F32),
            vmem((layers, heads * tiles, rows, 128), F32),
            vmem((layers, rows, width), F32),
            vmem((layers, heads, rows), F32),
            vmem((layers, rows, width), F32),
            vmem((layers, rows, width), F32),
            vmem((HEAD, HEAD * HEAD), BF16),
            vmem((layers, n, rows, width), BF16),
            vmem((layers, n, rows, block), F32),
            vmem((layers, n, rows, block), F32),
            vmem((layers, n, rows, block), BF16),
            vmem((layers, n // 2, rows, block), BF16),
            vmem((layers, n, rows, width), BF16),
            vmem((layers, n, rows, width), BF16),
            vmem((layers, 2, n, rows, width), BF16),
            pltpu.SemaphoreType.DMA((13,)),
            pltpu.SemaphoreType.DMA((layers, n)),
            pltpu.SemaphoreType.DMA((layers, n)),
            pltpu.SemaphoreType.DMA((layers,)),
            pltpu.SemaphoreType.DMA((layers, n)),
            pltpu.SemaphoreType.DMA((layers, 2)),
            pltpu.SemaphoreType.DMA((layers, 6)),
            pltpu.SemaphoreType.DMA((n,)),
            pltpu.SemaphoreType.REGULAR((n,)),
            pltpu.SemaphoreType.REGULAR,
        ],
        compiler_params=pltpu.CompilerParams(
            collective_id=0, has_side_effects=True, vmem_limit_bytes=48 * 1024 * 1024
        ),
        name="cells",
    )(
        *(
            pltpu.with_memory_space_constraint(a, pltpu.HBM)
            for a in (
                tokens,
                norm_gain,
                query_weight,
                key_weight,
                value_weight,
                outgate_weight,
                jnp.swapaxes(input_gate_weight, 1, 2),
                jnp.swapaxes(forget_gate_weight, 1, 2),
                forget_bias,
                out_weight,
                memory,
                normalizer_state,
                jnp.swapaxes(maximum_state, 1, 2),
            )
        )
    )
    results = (tokens_out, memory, normalizer, maximum)
    tokens_out, memory, normalizer, maximum = pl.pallas_call(
        put_out,
        out_shape=tuple(jax.ShapeDtypeStruct(r.shape, r.dtype) for r in results),
        in_specs=[in_vmem] * 4,
        out_specs=(in_hbm,) * 4,
        scratch_shapes=[pltpu.SemaphoreType.DMA((11,))],
        compiler_params=pltpu.CompilerParams(vmem_limit_bytes=4 * 1024 * 1024),
        name="put_out",
    )(*results)
    memory = memory.reshape(layers, rows, tiles, heads, 128).transpose(0, 1, 3, 2, 4)
    return (
        tokens_out,
        memory.reshape(layers, rows, heads, HEAD * HEAD),
        normalizer,
        jnp.swapaxes(maximum, 1, 2),
    )


def solution(mesh):
    n = mesh.shape["tp"]
    assert mesh.shape["dp"] == n
    in_specs = (
        P(("grp", "tp"), "dp"),
        P(None, "dp"),
        P(None, "dp", "tp"),
        P(None, "dp", "tp"),
        P(None, "dp", "tp"),
        P(None, "dp", "tp"),
        P(None, "dp", "tp"),
        P(None, "dp", "tp"),
        P(None, "tp"),
        P(None, "tp", "dp"),
        P(None, ("grp", "dp"), "tp", None),
        P(None, ("grp", "dp"), "tp"),
        P(None, ("grp", "dp"), "tp"),
    )
    out_specs = (
        P(("grp", "tp"), "dp"),
        P(None, ("grp", "dp"), "tp", None),
        P(None, ("grp", "dp"), "tp"),
        P(None, ("grp", "dp"), "tp"),
    )
    return jax.shard_map(
        functools.partial(per_device, n),
        mesh=mesh,
        in_specs=in_specs,
        out_specs=out_specs,
        check_vma=False,
    )
```

```python
import functools

import jax
import jax.numpy as jnp
from jax import lax
from jax.experimental import pallas as pl
from jax.experimental.pallas import tpu as pltpu
from jax.sharding import PartitionSpec as P

HEAD = 64
EPS = 1e-06
BATCH = 4
HUB = 1
MESH = pl.DeviceIdType.MESH
F32 = jnp.float32
BF16 = jnp.bfloat16


def dot(a, b):
    return lax.dot_general(a, b, (((1,), (0,)), ((), ())), preferred_element_type=F32)


def lane_iota(shape):
    return lax.broadcasted_iota(jnp.int32, shape, 1)


def kernel(
    n,
    layers,
    tok_h,
    gain_h,
    qw_h,
    kw_h,
    vw_h,
    ow_h,
    ig_h,
    fg_h,
    fb_h,
    pw_h,
    mem_h,
    nrm_h,
    mx_h,
    tok_o,
    mem_o,
    nrm_o,
    mx_o,
    gain,
    w,
    gate_in,
    gate_w,
    fb,
    pw,
    mem,
    mem_t,
    nrm,
    mx,
    old_max,
    bias,
    spread,
    xall,
    pfull,
    pother,
    psend,
    precv,
    mixall,
    osend,
    orecv,
    load_sem,
    x_sem,
    c_sem,
    p_sem,
    m_sem,
    o_sem,
    send_sem,
    hub_sem,
    plane_sem,
    ready_sem,
):
    tp = lax.axis_index("tp")
    dp = lax.axis_index("dp")
    rows, width = tok_h.shape
    heads = width // HEAD
    pairs = width // 128
    tiles = HEAD * HEAD // 128
    cols = 4 * width

    def dp_peer(i):
        return lax.rem(dp + i, n)

    def by_distance(i):
        half = lax.div(i + 1, 2)
        return lax.rem(tp + n + half * (2 * lax.rem(i, 2) - 1), n)

    def arrival(i):
        return lax.select(i < n - 2, HUB + i, lax.select(i == n - 2, 0, n - 1))

    core = lax.rem(dp, 2)
    chip = lax.div(dp, 2)
    sibling = dp + 1 - 2 * core
    odd = lax.rem(tp + core, 2)

    def batch_of(l, k):
        places = range(k * BATCH, (k + 1) * BATCH)
        if l == 0:
            return [arrival(i) for i in places]
        return [by_distance(i) for i in places]

    def of_core(l, k, mine):
        if l == 0:
            order = [(HUB + i) % 2 if i < n - 2 else (0, 1)[i - n + 2] for i in range(n)]
            flag = core
        else:
            order = [((i + 1) // 2) % 2 for i in range(n)]
            flag = odd
        places = range(k * BATCH, (k + 1) * BATCH)
        even = [i for i in places if order[i] == 0]
        uneven = [i for i in places if order[i] == 1]
        flag = flag if mine else 1 - flag
        where = arrival if l == 0 else by_distance
        return [where(lax.select(flag == 0, e, u)) for e, u in zip(even, uneven, strict=True)]

    barrier = pltpu.get_barrier_semaphore()
    at_hub = tp == HUB

    @pl.when(at_hub)
    def _():
        def greet(i, carry):
            pl.semaphore_signal(barrier, inc=1, device_id={"dp": dp_peer(i)}, device_id_type=MESH)
            there = {"tp": lax.rem(tp + i, n)}
            pl.semaphore_signal(barrier, inc=1, device_id=there, device_id_type=MESH)
            return carry

        lax.fori_loop(1, n, greet, 0)

    loads = [
        pltpu.make_async_copy(tok_h, xall.at[0, tp], load_sem.at[0]),
        pltpu.make_async_copy(gain_h, gain, load_sem.at[1]),
        pltpu.make_async_copy(ig_h, gate_in.at[0], load_sem.at[2]),
        pltpu.make_async_copy(fg_h, gate_in.at[1], load_sem.at[3]),
        pltpu.make_async_copy(fb_h, fb, load_sem.at[4]),
        pltpu.make_async_copy(mx_h, mx, load_sem.at[5]),
        pltpu.make_async_copy(nrm_h, nrm, load_sem.at[6]),
    ]
    for i, ref in enumerate((qw_h, kw_h, vw_h, ow_h)):
        loads.append(pltpu.make_async_copy(ref, w.at[i], load_sem.at[7 + i]))
    loads.append(pltpu.make_async_copy(mem_h, mem, load_sem.at[11]))
    loads.append(pltpu.make_async_copy(pw_h, pw, load_sem.at[12]))
    for copy in loads:
        copy.start()

    with jax.named_scope("barrier"):
        pl.semaphore_wait(barrier, lax.select(at_hub, n - 1, 1))
        loads[0].wait()

    def row_copy(l, block, t, sem):
        return pltpu.make_async_remote_copy(
            src_ref=xall.at[l, block],
            dst_ref=xall.at[l, block],
            send_sem=sem,
            recv_sem=x_sem.at[l, block],
            device_id={"tp": t},
            device_id_type=MESH,
        )

    def wait_rows(l, block):
        with jax.named_scope(f"wait_x{l}"):
            here = xall.at[l, block]
            pltpu.make_async_copy(here, here, x_sem.at[l, block]).wait()

    def send_rows(l):
        def far_first(k, carry):
            row_copy(l, tp, by_distance(n - k), send_sem.at[l, 0]).start()
            return carry

        lax.fori_loop(1, n, far_first, 0, unroll=True)

    @pl.when(jnp.logical_not(at_hub))
    def _():
        row_copy(0, tp, HUB, send_sem.at[0, 0]).start()

    for c in range(HEAD * HEAD // 512):
        shape = (HEAD, 512)
        block = lane_iota(shape) + c * 512
        row = lax.broadcasted_iota(jnp.int32, shape, 0)
        hit = (block >= row * HEAD) & (block < row * HEAD + HEAD)
        spread[:, c * 512 : (c + 1) * 512] = jnp.where(hit, 1.0, 0.0).astype(BF16)
    for copy in loads[1:7]:
        copy.wait()
    lane = lane_iota((rows, 128))
    row8 = lax.broadcasted_iota(jnp.int32, (rows, 128), 0)
    low = lane < HEAD

    def per_head(values):
        wide = [jnp.broadcast_to(v, (rows, 128)) for v in values]
        return jnp.concatenate(
            [jnp.where(low, wide[2 * p], wide[2 * p + 1]) for p in range(pairs)], axis=1
        )

    def both_halves(x, h):
        part = x[:, (h // 2) * 128 : (h // 2 + 1) * 128]
        turned = pltpu.roll(part, HEAD, 1)
        return jnp.where(low, part, turned) if h % 2 == 0 else jnp.where(low, turned, part)

    eye = (lane_iota((rows, rows)) == lax.broadcasted_iota(jnp.int32, (rows, rows), 0))
    for l in range(layers):
        gate_w[l] = jnp.concatenate(
            [
                gate_in[0, l].astype(F32),
                gate_in[1, l].astype(F32),
                jnp.zeros((128 - 2 * heads, width), F32),
            ],
            axis=0,
        ).astype(BF16)
        old = mx[l]
        old_max[l] = per_head(
            [
                jnp.sum(
                    jnp.where(eye, jnp.broadcast_to(old[h : h + 1, :], (rows, rows)), 0.0),
                    axis=1,
                    keepdims=True,
                )
                for h in range(heads)
            ]
        )
        bias[l] = per_head(
            [jnp.broadcast_to(fb[l : l + 1, h : h + 1], (rows, 1)) for h in range(heads)]
        )

    for copy in loads[7:12]:
        copy.wait()

    for l in range(layers):

        def turn(r, carry):
            mem_t[l, r] = mem[l, pl.ds(r, rows, stride=heads * tiles), :]
            return carry

        lax.fori_loop(0, heads * tiles, turn, 0, unroll=8)

    @pl.when(at_hub)
    def _():
        def relay(j, carry):
            block = arrival(j + 1)
            wait_rows(0, block)

            def tell(i, c):
                there = {"dp": dp_peer(i)}
                pl.semaphore_signal(
                    plane_sem.at[block], inc=1, device_id=there, device_id_type=MESH
                )
                return c

            lax.fori_loop(1, n, tell, 0)

            def to_known(q, c):
                t = arrival(q)
                row_copy(0, block, t, hub_sem.at[t]).start()
                return c

            lax.fori_loop(1, j + 1, to_known, 0)

            def catch_up(q, c):
                row_copy(0, arrival(q), block, hub_sem.at[block]).start()
                return c

            lax.fori_loop(0, j + 1, catch_up, 0)

            @pl.when((j > 0) & (j < n - 2))
            def _():
                settle(j - 1)

            return carry

        def settle(j):
            t = arrival(j + 1)
            pl.semaphore_wait(plane_sem.at[t], n - 1)
            pl.semaphore_signal(ready_sem, inc=1, device_id={"tp": t}, device_id_type=MESH)

        lax.fori_loop(0, n - 1, relay, 0)
        settle(n - 2)
        settle(n - 3)

    loads[12].wait()

    for l in range(layers):
        gain_row = gain[l : l + 1, :]

        def project(k):
            sources = batch_of(l, k)
            for t in sources:
                @pl.when((t != tp) & jnp.logical_not(at_hub) if l == 0 else t != tp)
                def _(t=t):
                    wait_rows(l, t)

            x = jnp.concatenate([xall[l, t].astype(F32) for t in sources], axis=0)
            scaled = (x * gain_row).astype(BF16)
            square = jnp.sum(x * x, axis=1, keepdims=True)
            gates = lax.dot_general(
                scaled, gate_w[l], (((1,), (1,)), ((), ())), preferred_element_type=F32
            )
            gates = jnp.where(
                lane_iota(gates.shape) == 2 * heads, jnp.broadcast_to(square, gates.shape), gates
            )
            parts = [dot(scaled, w[q, l]) for q in range(4)] + [gates]
            for j, t in enumerate(sources):
                pfull[l, t] = jnp.concatenate(
                    [p[j * rows : (j + 1) * rows] for p in parts], axis=1
                )
        def give(k):
            for t in of_core(l, k, False):
                pltpu.make_async_remote_copy(
                    src_ref=pfull.at[l, t],
                    dst_ref=pother.at[l, t],
                    send_sem=send_sem.at[l, 4],
                    recv_sem=c_sem.at[l, t],
                    device_id={"dp": sibling},
                    device_id_type=MESH,
                ).start()

        def pass_on(k):
            for t in of_core(l, k, True):
                with jax.named_scope(f"wait_c{l}"):
                    there = pother.at[l, t]
                    pltpu.make_async_copy(there, there, c_sem.at[l, t]).wait()
                both = pfull[l, t] + pother[l, t]
                gates = both[:, cols:]
                upper = gates.astype(BF16).astype(F32)
                rest = pltpu.roll(gates - upper, 16, 1)
                gates = jnp.where(lane < 16, upper, rest)
                block = jnp.concatenate([both[:, :cols], gates], axis=1)
                psend[l, t] = block.astype(BF16)

                @pl.when(t == dp)
                def _(t=t):
                    precv[l, chip] = psend[l, t]

                @pl.when(t != dp)
                def _(t=t):
                    pltpu.make_async_remote_copy(
                        src_ref=psend.at[l, t],
                        dst_ref=precv.at[l, chip],
                        send_sem=send_sem.at[l, 1],
                        recv_sem=p_sem.at[l],
                        device_id={"dp": t},
                        device_id_type=MESH,
                    ).start()

        last = n // BATCH - 1
        if l == 0:
            for k in range(last):
                project(k)
            late = tp == n - 1

            @pl.when(late)
            def _():
                project(last)

            @pl.when(jnp.logical_not(at_hub))
            def _():
                with jax.named_scope("ready"):
                    pl.semaphore_wait(ready_sem, 1)

            @pl.when(late)
            def _():
                give(last)

            for k in range(last):
                give(k)
            for k in range(last):
                pass_on(k)

            @pl.when(jnp.logical_not(late))
            def _():
                project(last)
                give(last)

        else:
            for k in range(last + 1):
                project(k)
                give(k)
                if k > 0:
                    pass_on(k - 1)
        pass_on(last)

        some = precv.at[l, pl.ds(0, n // 2 - 1)]
        with jax.named_scope(f"wait_p{l}"):
            pltpu.make_async_copy(some, some, p_sem.at[l]).wait()
        total = precv[l, 0].astype(F32)
        for s in range(1, n // 2):
            total = total + precv[l, s].astype(F32)
        gates = total[:, cols:]
        gates = gates + pltpu.roll(gates, 128 - 16, 1)
        inv_rms = lax.rsqrt(gates[:, 2 * heads : 2 * heads + 1] / (width * n) + EPS)
        gates = gates * inv_rms
        stored = (total[:, :cols] * inv_rms).astype(BF16).astype(F32)
        query = stored[:, :width]
        keys = stored[:, width : 2 * width] * HEAD**-0.5
        values = stored[:, 2 * width : 3 * width]
        outgate = stored[:, 3 * width :]

        def stack(x):
            return jnp.concatenate(
                [x[:, h * HEAD : (h + 1) * HEAD] for h in range(heads)], axis=0
            ).astype(BF16)

        query_rows = stack(query)
        acc = [None] * heads
        chunk = 4
        for c in range(tiles // chunk):
            wide = dot(query_rows, spread[:, c * chunk * 128 : (c + 1) * chunk * 128])
            for j in range(chunk):
                for h in range(heads):
                    term = (
                        wide[h * rows : (h + 1) * rows, j * 128 : (j + 1) * 128]
                        * mem_t[l, (c * chunk + j) * heads + h]
                    )
                    acc[h] = term if acc[h] is None else acc[h] + term

        input_pre = per_head([gates[:, h : h + 1] for h in range(heads)])
        forget_pre = per_head([gates[:, heads + h : heads + h + 1] for h in range(heads)]) + bias[l]
        log_forget = jnp.minimum(forget_pre, 0.0) - jnp.log1p(jnp.exp(-jnp.abs(forget_pre)))
        carried = log_forget + old_max[l]
        new_max = jnp.maximum(carried, input_pre)
        keep = jnp.exp(carried - new_max)
        admit = jnp.exp(input_pre - new_max)
        normalizer = keep * nrm[l] + admit * keys

        def head_sum(x):
            return per_head(
                [
                    jnp.sum(x[:, h * HEAD : (h + 1) * HEAD], axis=1, keepdims=True)
                    for h in range(heads)
                ]
            )

        query_key = head_sum(query * keys)
        denominator = head_sum(query * normalizer)
        folded = [a + pltpu.roll(a, HEAD, 1) for a in acc]
        from_memory = jnp.concatenate(
            [jnp.where(low, folded[2 * p], folded[2 * p + 1]) for p in range(pairs)], axis=1
        )
        numerator = keep * from_memory + admit * query_key * values
        readout = numerator / jnp.maximum(jnp.abs(denominator), jnp.exp(-new_max))
        mixall[l, dp] = (readout * jax.nn.sigmoid(outgate)).astype(BF16)

        def send_mixed(k, carry):
            half = lax.div(k, 2)
            i = lax.select(lax.rem(k, 2) == 0, n // 2 - half, n // 2 + half)
            pltpu.make_async_remote_copy(
                src_ref=mixall.at[l, dp],
                dst_ref=mixall.at[l, dp],
                send_sem=send_sem.at[l, 2],
                recv_sem=m_sem.at[l, dp],
                device_id={"dp": dp_peer(i)},
                device_id_type=MESH,
            ).start()
            return carry

        with jax.named_scope(f"send_m{l}"):
            lax.fori_loop(1, n, send_mixed, 0, unroll=True)

        nrm_o[l] = normalizer
        key_rows = stack(keys)
        keep_h = [both_halves(keep, h) for h in range(heads)]
        value_h = [both_halves(admit * values, h) for h in range(heads)]
        for h in range(heads):
            peak = jnp.where(lane == row8, both_halves(new_max, h), 0.0)
            mx_o[l, h : h + 1, :] = jnp.sum(peak, axis=0, keepdims=True)[:, :rows]
        for c in range(tiles // chunk):
            wide = dot(key_rows, spread[:, c * chunk * 128 : (c + 1) * chunk * 128])
            for j in range(chunk):
                for h in range(heads):
                    r = (c * chunk + j) * heads + h
                    spread_key = wide[h * rows : (h + 1) * rows, j * 128 : (j + 1) * 128]
                    mem_o[l, pl.ds(r, rows, stride=heads * tiles), :] = (
                        keep_h[h] * mem_t[l, r] + spread_key * value_h[h]
                    )

        def leave(k, carry):
            homes = [by_distance(k * BATCH + j) for j in range(BATCH)]
            if l == 0:
                homes = [
                    lax.select(tp == n - 1, by_distance(n - 1 - i), arrival(i))
                    for i in (k * BATCH + j for j in range(BATCH))
                ]
            for t in homes:

                @pl.when(t != dp)
                def _(t=t):
                    with jax.named_scope(f"wait_m{l}"):
                        here = mixall.at[l, t]
                        pltpu.make_async_copy(here, here, m_sem.at[l, t]).wait()

            mixed = jnp.concatenate([mixall[l, t].astype(F32) for t in homes], axis=0)
            part = dot(mixed.astype(BF16), pw[l])
            for j, t in enumerate(homes):
                osend[l, t] = part[j * rows : (j + 1) * rows].astype(BF16)
            for t in reversed(homes):

                @pl.when(t == tp)
                def _(t=t):
                    orecv[l, tp] = osend[l, t]

                @pl.when(t != tp)
                def _(t=t):
                    pltpu.make_async_remote_copy(
                        src_ref=osend.at[l, t],
                        dst_ref=orecv.at[l, tp],
                        send_sem=send_sem.at[l, 3],
                        recv_sem=o_sem.at[l],
                        device_id={"tp": t},
                        device_id_type=MESH,
                    ).start()

            return carry

        lax.fori_loop(0, n // BATCH, leave, 0)

        some = orecv.at[l, pl.ds(0, n - 1)]
        with jax.named_scope(f"wait_o{l}"):
            pltpu.make_async_copy(some, some, o_sem.at[l]).wait()
        total = orecv[l, 0].astype(F32)
        for s in range(1, n):
            total = total + orecv[l, s].astype(F32)
        rows_out = (xall[l, tp].astype(F32) + total).astype(BF16)
        if l + 1 < layers:
            xall[l + 1, tp] = rows_out
            send_rows(l + 1)
        else:
            tok_o[...] = rows_out

    for l in range(layers):
        sent = ((xall, n - 1), (psend, n // 2 - 1), (mixall, n - 1), (osend, n - 1), (pfull, n // 2))
        for k, (buffer, count) in enumerate(sent):
            some = buffer.at[l, pl.ds(0, count)]
            if l > 0 or k > 0:
                pltpu.make_async_copy(some, some, send_sem.at[l, k]).wait()

    @pl.when(jnp.logical_not(at_hub))
    def _():
        row_copy(0, tp, HUB, send_sem.at[0, 0]).wait_send()

    @pl.when(at_hub)
    def _():
        def handed_on(j, carry):
            some = xall.at[0, pl.ds(0, n - 1)]
            pltpu.make_async_copy(some, some, hub_sem.at[arrival(j + 1)]).wait()
            return carry

        lax.fori_loop(0, n - 1, handed_on, 0)


def put_out(*refs):
    sems = refs[8]
    pieces = 8
    copies = []
    for src, dst in zip(refs[:4], refs[4:8], strict=True):
        if src.ndim < 3 or src.shape[1] < 1024:
            copies.append((src, dst))
            continue
        step = src.shape[1] * src.shape[0] // pieces
        for at in range(0, src.shape[1], step):
            for l in range(src.shape[0]):
                copies.append((src.at[l, at : at + step], dst.at[l, at : at + step]))
    copies = [pltpu.make_async_copy(*c, sems.at[i]) for i, c in enumerate(copies)]
    for copy in copies:
        copy.start()
    for copy in copies:
        copy.wait()


def per_device(
    n,
    tokens,
    norm_gain,
    query_weight,
    key_weight,
    value_weight,
    outgate_weight,
    input_gate_weight,
    forget_gate_weight,
    forget_bias,
    out_weight,
    memory_state,
    normalizer_state,
    maximum_state,
):
    rows, width = tokens.shape
    layers = norm_gain.shape[0]
    heads = width // HEAD
    tiles = HEAD * HEAD // 128
    vmem = pltpu.VMEM

    memory = memory_state.reshape(layers, rows, heads, tiles, 128).transpose(0, 1, 3, 2, 4)
    memory = memory.reshape(layers, rows * tiles * heads, 128)

    in_hbm = pl.BlockSpec(memory_space=pltpu.HBM)
    in_vmem = pl.BlockSpec(memory_space=pltpu.VMEM)
    block = 4 * width + 128
    tokens_out, memory, normalizer, maximum = pl.pallas_call(
        functools.partial(kernel, n, layers),
        out_shape=(
            pltpu.VMEM((rows, width), BF16),
            pltpu.VMEM(memory.shape, F32),
            pltpu.VMEM((layers, rows, width), F32),
            pltpu.VMEM((layers, heads, rows), F32),
        ),
        in_specs=[in_hbm] * 13,
        out_specs=(in_vmem,) * 4,
        scratch_shapes=[
            vmem((layers, width), F32),
            vmem((4, layers, width, width), BF16),
            vmem((2, layers, heads, width), BF16),
            vmem((layers, 128, width), BF16),
            vmem((layers, heads), F32),
            vmem((layers, width, width), BF16),
            vmem(memory.shape, F32),
            vmem((layers, heads * tiles, rows, 128), F32),
            vmem((layers, rows, width), F32),
            vmem((layers, heads, rows), F32),
            vmem((layers, rows, width), F32),
            vmem((layers, rows, width), F32),
            vmem((HEAD, HEAD * HEAD), BF16),
            vmem((layers, n, rows, width), BF16),
            vmem((layers, n, rows, block), F32),
            vmem((layers, n, rows, block), F32),
            vmem((layers, n, rows, block), BF16),
            vmem((layers, n // 2, rows, block), BF16),
            vmem((layers, n, rows, width), BF16),
            vmem((layers, n, rows, width), BF16),
            vmem((layers, n, rows, width), BF16),
            pltpu.SemaphoreType.DMA((13,)),
            pltpu.SemaphoreType.DMA((layers, n)),
            pltpu.SemaphoreType.DMA((layers, n)),
            pltpu.SemaphoreType.DMA((layers,)),
            pltpu.SemaphoreType.DMA((layers, n)),
            pltpu.SemaphoreType.DMA((layers,)),
            pltpu.SemaphoreType.DMA((layers, 5)),
            pltpu.SemaphoreType.DMA((n,)),
            pltpu.SemaphoreType.REGULAR((n,)),
            pltpu.SemaphoreType.REGULAR,
        ],
        compiler_params=pltpu.CompilerParams(
            collective_id=0, has_side_effects=True, vmem_limit_bytes=48 * 1024 * 1024
        ),
        name="cells",
    )(
        *(
            pltpu.with_memory_space_constraint(a, pltpu.HBM)
            for a in (
                tokens,
                norm_gain,
                query_weight,
                key_weight,
                value_weight,
                outgate_weight,
                jnp.swapaxes(input_gate_weight, 1, 2),
                jnp.swapaxes(forget_gate_weight, 1, 2),
                forget_bias,
                out_weight,
                memory,
                normalizer_state,
                jnp.swapaxes(maximum_state, 1, 2),
            )
        )
    )
    results = (tokens_out, memory, normalizer, maximum)
    tokens_out, memory, normalizer, maximum = pl.pallas_call(
        put_out,
        out_shape=tuple(jax.ShapeDtypeStruct(r.shape, r.dtype) for r in results),
        in_specs=[in_vmem] * 4,
        out_specs=(in_hbm,) * 4,
        scratch_shapes=[pltpu.SemaphoreType.DMA((11,))],
        compiler_params=pltpu.CompilerParams(vmem_limit_bytes=4 * 1024 * 1024),
        name="put_out",
    )(*results)
    memory = memory.reshape(layers, rows, tiles, heads, 128).transpose(0, 1, 3, 2, 4)
    return (
        tokens_out,
        memory.reshape(layers, rows, heads, HEAD * HEAD),
        normalizer,
        jnp.swapaxes(maximum, 1, 2),
    )


def solution(mesh):
    n = mesh.shape["tp"]
    assert mesh.shape["dp"] == n
    in_specs = (
        P(("grp", "tp"), "dp"),
        P(None, "dp"),
        P(None, "dp", "tp"),
        P(None, "dp", "tp"),
        P(None, "dp", "tp"),
        P(None, "dp", "tp"),
        P(None, "dp", "tp"),
        P(None, "dp", "tp"),
        P(None, "tp"),
        P(None, "tp", "dp"),
        P(None, ("grp", "dp"), "tp", None),
        P(None, ("grp", "dp"), "tp"),
        P(None, ("grp", "dp"), "tp"),
    )
    out_specs = (
        P(("grp", "tp"), "dp"),
        P(None, ("grp", "dp"), "tp", None),
        P(None, ("grp", "dp"), "tp"),
        P(None, ("grp", "dp"), "tp"),
    )
    return jax.shard_map(
        functools.partial(per_device, n),
        mesh=mesh,
        in_specs=in_specs,
        out_specs=out_specs,
        check_vma=False,
    )
```
